32 devices in a mesh: ep: 4 (over y, x), tp: 8 (over z, core).
Axes of the slice: x: 2, y: 2, z: 4, core: 2. Of those that a mesh axis runs over, the one named last changes fastest.
Arguments:
- query_heads_rows: bfloat16 [2048, 2048], P('ep', 'tp'), may hold values from -9 to 9
- key_heads_rows: bfloat16 [2048, 2048], P('ep', 'tp'), may hold values from -9 to 9
- value_heads_rows: bfloat16 [2048, 2048], P('ep', 'tp'), may hold values from -6 to 6
- write_strength_logit: bfloat16 [16, 2048], P('tp', 'ep'), may hold values from -3.5 to -1
- decay_preactivation: bfloat16 [16, 2048], P('tp', 'ep'), may hold values from -5 to 5
- head_decay_logarithm: float32 [16], P('tp'), may hold values from -20 to -3
- extra_log_decay: float32 [16, 2048], P('tp', 'ep'), may hold values from -0.7 to 0
- output_weight: bfloat16 [2048, 2048], P('tp'), may hold values from -2 to 2
- second_batch_tokens: bfloat16 [4096, 2048], P(('ep', 'tp')), may hold values from -6 to 6
- expert_norm_scale: float32 [2048], replicated, may hold values from 0.1 to 1.9
- expert_choice_index: int32 [4096, 2], P(('ep', 'tp')), may hold values from 0 to 15, as said below
- group_router_weight: float32 [4096], P(('ep', 'tp')), may hold values from 0.25 to 1
- expert_logit_difference: float32 [4096], P(('ep', 'tp')), may hold values from -8 to 8
- expert_gate_weight: bfloat16 [16, 1024, 2048], P('ep', 'tp'), may hold values from -0.125 to 0.125
- expert_up_weight: bfloat16 [16, 1024, 2048], P('ep', 'tp'), may hold values from -0.125 to 0.125
- expert_down_weight: bfloat16 [16, 1024, 2048], P('ep', 'tp'), may hold values from -0.375 to 0.375
Outputs:
- mixer_output_first: bfloat16 [2048, 2048], P(('ep', 'tp'))
- expert_out: bfloat16 [4096, 2048], P(('ep', 'tp'))
The draws below stay inside these ranges and needn't reach their ends.
Inputs may be any that keep to these rules, and one draw needn't show every extreme that they name: `expert_choice_index`: each row names two different experts of one group, the experts a * 4 to a * 4 + 3 for some a. In the rows of one device (aligned blocks of 128 rows) no expert is named more than 32 times, and in every device's rows some expert is named exactly 32 times.
All inputs are finite; a program needn't handle non-finite values.
Results may differ from the reference program's by a relative error of at most 0.018.
Values may be sent and summed in bfloat16 or wider, within the bound.
A program may use at most 128 MiB of HBM per device.

```python
import jax
import jax.numpy as jnp
from jax import lax

D = 2048
HEADS = 16
DK = 128
DV = 128
BLOCK = 64
TOK_AEP = 512
SEQ = 2048
TOK_B = 128
CAP = 32
TOKENS_B = 4096
FF = 1024
EXPERTS = 16
GROUPS = 4
EPG = 4
TOPK = 2


def shared_directions(key):
    return jax.random.truncated_normal(jax.random.fold_in(key, 71), -3.0, 3.0, (HEADS, DK))


def coherent_rows(key, salt, lowest, highest):
    level_key, noise_key = jax.random.split(jax.random.fold_in(key, salt))
    direction = shared_directions(key)
    noise = jax.random.truncated_normal(noise_key, -3.0, 3.0, (SEQ, HEADS, DK))
    levels = jax.random.uniform(level_key, (SEQ // BLOCK, HEADS), minval=lowest, maxval=highest)
    per_position = jnp.repeat(levels, BLOCK, axis=0)
    rows = per_position[:, :, None] * direction[None, :, :] + noise
    return rows.reshape(SEQ, HEADS * DK).astype(jnp.bfloat16)


def draw_query_heads_rows(key, part):
    return coherent_rows(key, 13, 0.8, 1.2)


def draw_key_heads_rows(key, part):
    return coherent_rows(key, 12, 1.2, 1.8)


def draw_head_decay_logarithm(key, part):
    pick_key, slow_key, fast_key = jax.random.split(key, 3)
    slow_share = 0.5
    chosen = jax.random.uniform(pick_key, (HEADS,)) < slow_share
    slow_rate = jnp.log(jnp.log(10.0) / (2.4 * SEQ)) + jax.random.uniform(slow_key, (HEADS,), minval=-0.3, maxval=0.3)
    fast_rate = jnp.log(1.0 / 32.0) + jax.random.uniform(fast_key, (HEADS,), minval=-0.3, maxval=0.3)
    return jnp.where(chosen, slow_rate, fast_rate).astype(jnp.float32)


def draw_decay_preactivation(key, part):
    jitter_key, device_key, block_key, run_key = jax.random.split(key, 4)
    segments_count = SEQ // TOK_AEP
    jitter = 0.5 * jax.random.truncated_normal(jitter_key, -3.0, 3.0, (HEADS, SEQ))
    per_device = jax.random.uniform(device_key, (segments_count,), minval=-1.5, maxval=1.5)
    run_start = jax.random.randint(run_key, (), 0, max(segments_count - 2, 1))
    segment_index = jnp.arange(segments_count, dtype=jnp.int32)
    in_run = (segment_index >= run_start) & (segment_index < run_start + 3)
    per_device = jnp.where(in_run, -3.0, per_device)
    per_block = jax.random.uniform(block_key, (SEQ // BLOCK,), minval=-0.5, maxval=0.5)
    offsets = jnp.repeat(per_device, TOK_AEP) + jnp.repeat(per_block, BLOCK)
    return jnp.clip(jitter + offsets[None, :], -5.0, 5.0).astype(jnp.bfloat16)


def draw_extra_log_decay(key, part):
    place_key, depth_key = jax.random.split(key)
    half_length = SEQ // 2
    places = jax.random.randint(place_key, (HEADS, 2), 0, half_length) + jnp.array([0, half_length], jnp.int32)[None, :]
    depths = jnp.log(jax.random.uniform(depth_key, (HEADS, 2), minval=0.5, maxval=0.8))
    positions = jnp.arange(SEQ, dtype=jnp.int32)
    markers = (positions[None, None, :] == places[:, :, None]).astype(jnp.float32)
    return jnp.sum(markers * depths[:, :, None], axis=1).astype(jnp.float32)


def route_block(block_key):
    hot_key, split_key, order_key = jax.random.split(block_key, 3)
    hot_rows = EPG * CAP // 2
    hot_group = jax.random.randint(hot_key, (), 0, GROUPS)
    remain = jnp.asarray(TOK_B - hot_rows, jnp.int32)
    split_keys = jax.random.split(split_key, GROUPS - 1)
    others = []
    for number in range(GROUPS - 2):
        lowest = jnp.maximum(0, remain - hot_rows * (GROUPS - 2 - number))
        highest = jnp.minimum(hot_rows, remain)
        counted = jax.random.randint(split_keys[number], (), lowest, highest + 1).astype(jnp.int32)
        others.append(counted)
        remain = remain - counted
    others.append(remain)
    other_counts = jnp.stack(others).astype(jnp.int32)
    group_index = jnp.arange(GROUPS, dtype=jnp.int32)
    shifted = jnp.clip(group_index - (group_index > hot_group).astype(jnp.int32), 0, GROUPS - 2)
    counts = jnp.where(group_index == hot_group, hot_rows, other_counts[shifted]).astype(jnp.int32)
    group_ends = jnp.cumsum(counts)
    starts = group_ends - counts
    places = jax.random.permutation(order_key, TOK_B).astype(jnp.int32)
    groups = jnp.sum((places[:, None] >= group_ends[None, :]).astype(jnp.int32), axis=1)
    within = places - starts[groups]
    first_id = groups * EPG + within % EPG
    second = groups * EPG + (within + 1 + within // EPG % (EPG - 1)) % EPG
    return jnp.stack([first_id, second], axis=1).astype(jnp.int32)


def draw_expert_choice_index(key, part):
    block_keys = jax.random.split(key, TOKENS_B // TOK_B)
    return jax.vmap(route_block)(block_keys).reshape(TOKENS_B, TOPK).astype(jnp.int32)


def shard_levels(rng, shape, cuts, smallest, top_value):
    loudness, own = 1.0, jax.random.fold_in(rng, 6)
    for dim, blocks in cuts:
        draws = jnp.exp(jax.random.uniform(jax.random.fold_in(own, dim), (blocks,), jnp.float32, smallest / len(cuts), top_value / len(cuts)))
        loudness = loudness * jnp.repeat(draws, shape[dim] // blocks).reshape([-1 if axis == dim else 1 for axis in range(len(shape))])
    return loudness


def normal_values(own_key, extent, deviation, bound, cuts=(), kind=jnp.bfloat16):
    factor_of = shard_levels(own_key, extent, cuts, -0.22, 0.18) if cuts else 1.0
    drawn = jax.random.normal(own_key, extent, jnp.float32) * deviation * factor_of
    return jnp.minimum(jnp.maximum(drawn, -bound), bound).astype(kind)


def setup_inputs(seed: int = 0) -> dict:
    key_of = jax.random.split(jax.random.key(seed), 17)
    query_heads_rows = draw_query_heads_rows(jax.random.fold_in(key_of[16], 71), 0)
    key_heads_rows = draw_key_heads_rows(jax.random.fold_in(key_of[16], 71), 0)
    value_heads_rows = normal_values(key_of[2], (SEQ, HEADS * DV), 1.0, 6.0, ((0, 4), (1, 8)))
    write_strength_logit = jnp.clip(-3.5 + 2.5 * jax.random.uniform(key_of[3], (HEADS, SEQ), jnp.float32) ** shard_levels(key_of[3], (HEADS, SEQ), ((0, 8), (1, 4)), -0.2, 0.2), -3.5, -1.0).astype(jnp.bfloat16)
    decay_preactivation = draw_decay_preactivation(jax.random.fold_in(key_of[16], 71), 0)
    head_decay_logarithm = draw_head_decay_logarithm(jax.random.fold_in(key_of[16], 71), 0)
    extra_log_decay = draw_extra_log_decay(jax.random.fold_in(key_of[16], 71), 0)
    output_weight = normal_values(key_of[7], (HEADS * DV, D), ((HEADS * DV) // 256) ** -0.5, 2.0, ((0, 8),))
    second_batch_tokens = normal_values(key_of[8], (TOKENS_B, D), 1.0, 6.0, ((0, 32),))
    expert_norm_scale = jnp.clip(1.0 + 0.18 * jax.random.normal(key_of[9], (D,), jnp.float32), 0.1, 1.9)
    expert_choice_index = draw_expert_choice_index(jax.random.fold_in(key_of[16], 71), 0)
    group_router_weight = jnp.clip(0.25 + 0.75 * jax.random.uniform(key_of[11], (TOKENS_B,), jnp.float32) ** shard_levels(key_of[11], (TOKENS_B,), ((0, 32),), -0.2, 0.2), 0.25, 1.0)
    expert_logit_difference = normal_values(key_of[12], (TOKENS_B,), 1.5, 8.0, ((0, 32),), jnp.float32)
    expert_gate_weight = normal_values(key_of[13], (EXPERTS, FF, D), D ** -0.5, 0.125, ((0, 4), (1, 8)))
    expert_up_weight = normal_values(key_of[14], (EXPERTS, FF, D), D ** -0.5, 0.125, ((0, 4), (1, 8)))
    expert_down_weight = normal_values(key_of[15], (EXPERTS, FF, D), (FF // 4) ** -0.5, 0.375, ((0, 4), (1, 8)))
    return dict(query_heads_rows=query_heads_rows, key_heads_rows=key_heads_rows, value_heads_rows=value_heads_rows, write_strength_logit=write_strength_logit, decay_preactivation=decay_preactivation, head_decay_logarithm=head_decay_logarithm, extra_log_decay=extra_log_decay, output_weight=output_weight, second_batch_tokens=second_batch_tokens, expert_norm_scale=expert_norm_scale, expert_choice_index=expert_choice_index, group_router_weight=group_router_weight, expert_logit_difference=expert_logit_difference, expert_gate_weight=expert_gate_weight, expert_up_weight=expert_up_weight, expert_down_weight=expert_down_weight)


precise_setting = lax.Precision.HIGHEST
norm_eps = 1e-06

def unit_rows(matrix):
    return matrix * lax.rsqrt(lax.optimization_barrier(jnp.sum(matrix * matrix, axis=-1, keepdims=True)) + norm_eps)

def block_terms(query_block, key_block, value_block, decay_logarithm, strength):
    span_len = query_block.shape[2]
    dim_value = value_block.shape[-1]
    cumulative = jnp.cumsum(decay_logarithm, axis=-1)
    within = jnp.tril(jnp.ones((span_len, span_len), bool))
    strict = jnp.tril(jnp.ones((span_len, span_len), bool), -1)
    spread = cumulative[..., :, None] - cumulative[..., None, :]
    decayed = jnp.where(within, jnp.exp(jnp.where(within, spread, 0.0)), 0.0)
    weighted = key_block * strength[..., None]
    lower_part = jnp.where(strict, jnp.einsum('hnid,hnjd->hnij', weighted, key_block, precision=precise_setting) * decayed, 0.0)
    system = lower_part + jnp.eye(span_len, dtype=jnp.float32)
    rhs_cols = jnp.concatenate([value_block * strength[..., None], weighted * jnp.exp(cumulative)[..., None]], axis=-1)
    solved = jax.scipy.linalg.solve_triangular(system, rhs_cols, lower=True, unit_diagonal=True)
    updated_values = solved[..., :dim_value]
    delta_corrections = solved[..., dim_value:]
    scores = jnp.where(within, jnp.einsum('hnid,hnjd->hnij', query_block, key_block, precision=precise_setting) * decayed, 0.0)
    decayed_queries = query_block * jnp.exp(cumulative)[..., None]
    decayed_keys = key_block * jnp.exp(cumulative[..., -1:] - cumulative)[..., None]
    block_retention = jnp.exp(cumulative[..., -1])
    return (decayed_queries, decayed_keys, updated_values, delta_corrections, scores, block_retention)

def carry_step(recurrent_state, inputs):
    decayed_queries, decayed_keys, updated_values, delta_corrections, scores, block_retention = inputs
    value_updates = updated_values - jnp.einsum('jdb,jbu->jdu', delta_corrections, recurrent_state, precision=precise_setting)
    final_output = jnp.einsum('jdb,jbu->jdu', decayed_queries, recurrent_state, precision=precise_setting)
    final_output = final_output + jnp.einsum('hcj,hjv->hcv', scores, value_updates, precision=precise_setting)
    recurrent_state = recurrent_state * block_retention[:, None, None] + jnp.einsum('rpq,rpd->rqd', decayed_keys, value_updates, precision=precise_setting)
    return (recurrent_state, final_output)

def mixer_portion(query_heads_rows, key_heads_rows, value_heads_rows, write_strength_logit, decay_preactivation, head_decay_logarithm, extra_log_decay, output_weight):
    length = query_heads_rows.shape[0]
    blocks = length // BLOCK

    def heads_first(matrix):
        spread_out = matrix.astype(jnp.float32).reshape(length, HEADS, -1).transpose(1, 0, 2)
        return spread_out.reshape(HEADS, blocks, BLOCK, -1)
    query_block = unit_rows(heads_first(query_heads_rows)) * DK ** (-0.5)
    key_block = unit_rows(heads_first(key_heads_rows))
    value_block = heads_first(value_heads_rows)
    strength = jax.nn.sigmoid(write_strength_logit.astype(jnp.float32)).reshape(HEADS, blocks, BLOCK)
    decay_logarithm = -jnp.exp(head_decay_logarithm)[:, None] * jax.nn.softplus(decay_preactivation.astype(jnp.float32)) + extra_log_decay
    decay_logarithm = decay_logarithm.reshape(HEADS, blocks, BLOCK)
    terms = block_terms(query_block, key_block, value_block, decay_logarithm, strength)
    inputs = tuple((jnp.moveaxis(term, 1, 0) for term in terms))
    _, outputs = lax.scan(carry_step, jnp.zeros((HEADS, DK, DV), jnp.float32), inputs)
    attention_result = outputs.transpose(0, 2, 1, 3).reshape(length, HEADS * DV).astype(jnp.bfloat16)
    return jnp.dot(attention_result.astype(jnp.float32), output_weight.astype(jnp.float32), preferred_element_type=jnp.float32).astype(jnp.bfloat16)

def experts_part(second_batch_tokens, expert_norm_scale, expert_choice_index, group_router_weight, expert_logit_difference, expert_gate_weight, expert_up_weight, expert_down_weight):
    widened = second_batch_tokens.astype(jnp.float32)
    normed = (widened * lax.rsqrt(lax.optimization_barrier(jnp.mean(widened * widened, axis=-1, keepdims=True)) + norm_eps) * expert_norm_scale).astype(jnp.bfloat16)
    token_count = second_batch_tokens.shape[0]
    width_model = second_batch_tokens.shape[1]
    flat_ids = expert_choice_index.reshape(-1).astype(jnp.int32)
    copy_count = flat_ids.shape[0]
    sorted_order = jnp.argsort(flat_ids, stable=True).astype(jnp.int32)
    sorted_ids = flat_ids[sorted_order]
    counts = lax.optimization_barrier(jnp.sum((flat_ids[:, None] == jnp.arange(EXPERTS, dtype=jnp.int32)[None, :]).astype(jnp.int32), axis=0))
    starts = jnp.cumsum(counts) - counts
    padded = (counts + 127) // 128 * 128
    pad_ends = jnp.cumsum(padded)
    pad_starts = pad_ends - padded
    destination = (pad_starts[sorted_ids] + jnp.arange(copy_count, dtype=jnp.int32) - starts[sorted_ids]).astype(jnp.int32)
    segments = -(-copy_count // 128) + EXPERTS
    source = jnp.full((segments * 128,), token_count, jnp.int32).at[destination].set((sorted_order // TOPK).astype(jnp.int32))
    padded_rows = jnp.concatenate([normed, jnp.zeros((1, width_model), jnp.bfloat16)], axis=0)
    gathered = padded_rows[source]
    seg_expert = jnp.minimum(jnp.searchsorted(pad_ends, jnp.arange(segments, dtype=jnp.int32) * 128, side='right'), EXPERTS - 1).astype(jnp.int32)

    def one_segment(operands):
        segment_rows, expert = operands
        gating = jnp.dot(segment_rows.astype(jnp.float32), expert_gate_weight[expert].T.astype(jnp.float32), preferred_element_type=jnp.float32)
        upward = jnp.dot(segment_rows.astype(jnp.float32), expert_up_weight[expert].T.astype(jnp.float32), preferred_element_type=jnp.float32)
        hidden = (jax.nn.silu(gating) * upward).astype(jnp.bfloat16)
        return jnp.dot(hidden.astype(jnp.float32), expert_down_weight[expert].astype(jnp.float32), preferred_element_type=jnp.float32).astype(jnp.bfloat16)
    results = lax.map(one_segment, (gathered.reshape(segments, 128, width_model), seg_expert))
    per_copy = results.reshape(-1, width_model)[destination]
    unsorted = jnp.zeros((copy_count, width_model), jnp.bfloat16).at[sorted_order].set(per_copy)
    copies = unsorted.reshape(token_count, TOPK, width_model).astype(jnp.float32)
    leading = jax.nn.sigmoid(expert_logit_difference)
    weights = group_router_weight[:, None] * jnp.stack([leading, 1.0 - leading], axis=-1)
    return lax.optimization_barrier(jnp.sum(weights[..., None] * copies, axis=1)).astype(jnp.bfloat16)

def reference(query_heads_rows, key_heads_rows, value_heads_rows, write_strength_logit, decay_preactivation, head_decay_logarithm, extra_log_decay, output_weight, second_batch_tokens, expert_norm_scale, expert_choice_index, group_router_weight, expert_logit_difference, expert_gate_weight, expert_up_weight, expert_down_weight):
    mixer_output_first = mixer_portion(query_heads_rows, key_heads_rows, value_heads_rows, write_strength_logit, decay_preactivation, head_decay_logarithm, extra_log_decay, output_weight)
    expert_out = experts_part(second_batch_tokens, expert_norm_scale, expert_choice_index, group_router_weight, expert_logit_difference, expert_gate_weight, expert_up_weight, expert_down_weight)
    return (mixer_output_first, expert_out)
```

```python
import jax
import jax.numpy as jnp
from jax import lax
from jax.experimental import pallas as pl
from jax.experimental.pallas import tpu as pltpu
from jax.sharding import PartitionSpec as P

DK = 128
DV = 128
CAP = 32
EPG = 4
TOPK = 2


precise_setting = lax.Precision.HIGHEST
norm_eps = 1e-06


def prefix(value, axis, join, neutral):
    count, mine = (lax.axis_size(axis), lax.axis_index(axis))
    pieces = jax.tree.map(lambda part: lax.all_gather(part, axis), value)
    subtotal = jax.tree.map(
        lambda part, zero: jnp.full_like(part, 0) + jnp.asarray(zero, part.dtype), value, neutral
    )

    def step(position, subtotal):
        longer = join(subtotal, jax.tree.map(lambda part: part[position], pieces))
        return jax.tree.map(lambda new, old: jnp.where(position < mine, new, old), longer, subtotal)

    return lax.fori_loop(0, count - 1, step, subtotal)


def unit_rows(matrix):
    return matrix * lax.rsqrt(jnp.sum(matrix * matrix, axis=-1, keepdims=True) + norm_eps)


def mm(a, b, dims=((1,), (0,))):
    return lax.dot_general(
        a, b, (dims, ((), ())), precision=precise_setting, preferred_element_type=jnp.float32
    )


def delta_kernel(q_ref, k_ref, v_ref, strength_ref, decay_ref, local_ref, proj_ref, end_ref):
    heads = strength_ref.shape[0]
    chunk = DK
    chunks = q_ref.shape[0] // chunk
    rows = lax.broadcasted_iota(jnp.int32, (chunk, chunk), 0)
    cols = lax.broadcasted_iota(jnp.int32, (chunk, chunk), 1)
    within = rows >= cols
    eye = jnp.where(rows == cols, 1.0, 0.0)
    parts = []
    for h in range(heads):
        for c in range(chunks):
            at = pl.ds(c * chunk, chunk)
            q = q_ref[at, h * DK : (h + 1) * DK].astype(jnp.float32)
            k = k_ref[at, h * DK : (h + 1) * DK].astype(jnp.float32)
            v = v_ref[at, h * DV : (h + 1) * DV].astype(jnp.float32)
            q = unit_rows(q) * DK ** (-0.5)
            k = unit_rows(k)
            d_row = decay_ref[h : h + 1, c * chunk : (c + 1) * chunk]
            b_row = strength_ref[h : h + 1, c * chunk : (c + 1) * chunk]
            d_col = jnp.sum(jnp.where(rows == cols, d_row, 0.0), axis=1, keepdims=True)
            b_col = jnp.sum(jnp.where(rows == cols, b_row, 0.0), axis=1, keepdims=True)
            cum_col = jnp.sum(jnp.where(within, d_row, 0.0), axis=1, keepdims=True)
            cum_row = jnp.sum(jnp.where(rows <= cols, d_col, 0.0), axis=0, keepdims=True)
            last = cum_col[chunk - 1 : chunk, :]
            decayed = jnp.where(within, jnp.exp(jnp.where(within, cum_col - cum_row, 0.0)), 0.0)
            weighted = k * b_col
            lower = jnp.where(
                rows > cols, mm(weighted, k, ((1,), (1,))) * decayed, 0.0
            )
            scores = mm(q, k, ((1,), (1,))) * decayed
            grown = jnp.exp(cum_col)
            rhs = jnp.concatenate([v * b_col, weighted * grown], axis=1)
            parts.append([lower, scores, rhs, q * grown, k * jnp.exp(last - cum_col), jnp.exp(last)])
    inverses = [None] * len(parts)
    span = 1
    while span < chunk:
        mask = (
            (rows // (2 * span) == cols // (2 * span))
            & (rows // span % 2 == 1)
            & (cols // span % 2 == 0)
        )
        for i, part in enumerate(parts):
            edge = jnp.where(mask, part[0], 0.0)
            if span == 1:
                inverses[i] = eye - edge
            else:
                inverses[i] = inverses[i] - mm(mm(inverses[i], edge), inverses[i])
        span *= 2
    solved = [mm(inverse, part[2]) for inverse, part in zip(inverses, parts)]
    states = [
        jnp.concatenate([jnp.zeros((DK, DV), jnp.float32), eye], axis=1) for _ in range(heads)
    ]
    for c in range(chunks):
        for h in range(heads):
            _, scores, _, queries, keys, retention = parts[h * chunks + c]
            both = solved[h * chunks + c]
            fresh = jnp.concatenate([both[:, :DV], jnp.zeros((chunk, DK), jnp.float32)], axis=1)
            state = states[h]
            updates = fresh - mm(both[:, DV:], state)
            out = mm(queries, state) + mm(scores, updates)
            states[h] = state * retention + mm(keys, updates, ((0,), (0,)))
            at = pl.ds(c * chunk, chunk)
            local_ref[h, at, :] = out[:, :DV]
            proj_ref[h, at, :] = out[:, DV:]
    for h in range(heads):
        end_ref[h] = states[h]


def delta_rule(queries, keys, values, strength, decay_logarithm):
    heads, length = strength.shape
    vmem = pl.BlockSpec(memory_space=pltpu.VMEM)
    f32 = jnp.float32
    return pl.pallas_call(
        delta_kernel,
        out_shape=(
            jax.ShapeDtypeStruct((heads, length, DV), f32),
            jax.ShapeDtypeStruct((heads, length, DK), f32),
            jax.ShapeDtypeStruct((heads, DK, DV + DK), f32),
        ),
        in_specs=[vmem] * 5,
        out_specs=(vmem,) * 3,
        cost_estimate=pl.CostEstimate(
            flops=40 * heads * length * DK * DK * 6, bytes_accessed=4 * 2**20, transcendentals=0
        ),
        compiler_params=pltpu.CompilerParams(vmem_limit_bytes=40 * 2**20),
    )(queries, keys, values, strength, decay_logarithm)


def expert_kernel(x_ref, gate_ref, up_ref, down_ref, out_ref):
    experts, units, width = gate_ref.shape
    x = x_ref[:, :width]
    hidden = []
    for e in range(experts):
        gating = lax.dot_general(
            x, gate_ref[e], (((1,), (1,)), ((), ())), preferred_element_type=jnp.float32
        )
        upward = lax.dot_general(
            x, up_ref[e], (((1,), (1,)), ((), ())), preferred_element_type=jnp.float32
        )
        share = x_ref[:, width + e : width + e + 1].astype(jnp.float32) + x_ref[
            :, width + experts + e : width + experts + e + 1
        ].astype(jnp.float32)
        hidden.append((gating / (1.0 + jnp.exp(-gating)) * upward * share).astype(jnp.bfloat16))
    hidden = jnp.concatenate(hidden, axis=1)
    down = down_ref[...].reshape(experts * units, width)
    out_ref[...] = jnp.dot(hidden, down, preferred_element_type=jnp.float32).astype(jnp.bfloat16)


def expert_layer(rows, gate, up, down, tile):
    count, wide = rows.shape
    experts, units, width = gate.shape
    whole = pl.BlockSpec((experts, units, width), lambda i: (0, 0, 0))
    return pl.pallas_call(
        expert_kernel,
        grid=(count // tile,),
        out_shape=jax.ShapeDtypeStruct((count, width), jnp.bfloat16),
        in_specs=[pl.BlockSpec((tile, wide), lambda i: (i, 0)), whole, whole, whole],
        out_specs=pl.BlockSpec((tile, width), lambda i: (i, 0)),
        cost_estimate=pl.CostEstimate(
            flops=6 * count * experts * units * width,
            bytes_accessed=4 * count * width + 6 * experts * units * width,
            transcendentals=0,
        ),
        compiler_params=pltpu.CompilerParams(vmem_limit_bytes=48 * 2**20),
    )(rows, gate, up, down)


def by_tokens(normed, choice, mixing, gate, up, down, slots):
    ep_count = lax.axis_size("ep")
    local_experts = gate.shape[0]
    tokens, width = normed.shape
    bf16 = jnp.bfloat16
    f32 = jnp.float32
    named = choice[:, :, None] == jnp.arange(ep_count * local_experts, dtype=jnp.int32)
    share = jnp.sum(jnp.where(named, mixing[:, :, None], 0.0), axis=1)
    goes = jnp.any(named, axis=1).reshape(tokens, ep_count, local_experts).any(axis=-1)
    earlier = jnp.tril(jnp.ones((tokens, tokens), bf16), -1)
    rank = jnp.dot(earlier, goes.astype(bf16), preferred_element_type=f32)
    spread = goes[:, :, None] & (rank[:, :, None] == jnp.arange(slots, dtype=f32))
    spread = spread.astype(bf16)
    high = share.astype(bf16)
    low = (share - high.astype(f32)).astype(bf16)
    sent = jnp.einsum("tes,td->esd", spread, normed, preferred_element_type=f32).astype(bf16)
    extra = jnp.concatenate(
        [
            high.reshape(tokens, ep_count, local_experts),
            low.reshape(tokens, ep_count, local_experts),
        ],
        axis=-1,
    )
    extra = jnp.einsum("tes,tex->esx", spread, extra, preferred_element_type=f32).astype(bf16)
    pad = -extra.shape[-1] % 128
    extra = jnp.pad(extra, ((0, 0), (0, 0), (0, pad)))
    outgoing = jnp.concatenate([sent, extra], axis=-1)
    arrived = lax.all_to_all(outgoing, "ep", split_axis=0, concat_axis=0, tiled=True)
    arrived = arrived.reshape(ep_count * slots, -1)
    everyone = lax.all_gather(arrived, "tp", axis=0, tiled=True)
    produced = expert_layer(everyone, gate, up, down, arrived.shape[0])
    summed = lax.psum_scatter(produced, "tp", scatter_dimension=0, tiled=True)
    returned = lax.all_to_all(
        summed.reshape(ep_count, slots, width), "ep", split_axis=0, concat_axis=0, tiled=True
    )
    return jnp.einsum("tes,esd->td", spread, returned, preferred_element_type=f32).astype(bf16)


def by_weights(normed, expert_choice_index, mixing, gate, up, down):
    own_tokens, width_model = normed.shape
    ep_count = lax.axis_size("ep")
    local_experts = gate.shape[0]
    experts = local_experts * ep_count
    flat_ids = expert_choice_index.reshape(-1)
    one_hot = (flat_ids[:, None] == jnp.arange(experts, dtype=jnp.int32)[None, :]).astype(jnp.int32)
    slot_rank = jnp.sum((jnp.cumsum(one_hot, axis=0) - one_hot) * one_hot, axis=1)
    slot_index = flat_ids * CAP + slot_rank
    copy_token = jnp.arange(flat_ids.shape[0], dtype=jnp.int32) // TOPK
    slot_token = jnp.full((experts * CAP,), own_tokens, jnp.int32).at[slot_index].set(copy_token)
    outgoing = jnp.take(normed, slot_token, axis=0, mode="fill", fill_value=0).reshape(
        ep_count, local_experts, CAP, width_model
    )
    arrived = lax.all_to_all(outgoing, "ep", split_axis=0, concat_axis=0, tiled=True)
    gate_piece = lax.all_gather(gate, "tp", axis=1, tiled=True)
    up_piece = lax.all_gather(up, "tp", axis=1, tiled=True)
    down_piece = lax.all_gather(down, "tp", axis=1, tiled=True)
    gating = jnp.einsum("secd,efd->secf", arrived, gate_piece, preferred_element_type=jnp.float32)
    upward = jnp.einsum("secd,efd->secf", arrived, up_piece, preferred_element_type=jnp.float32)
    hidden = (jax.nn.silu(gating) * upward).astype(jnp.bfloat16)
    produced = jnp.einsum("secf,efd->secd", hidden, down_piece, preferred_element_type=jnp.float32)
    returned = lax.all_to_all(
        produced.astype(jnp.bfloat16), "ep", split_axis=0, concat_axis=0, tiled=True
    )
    flat_results = returned.reshape(experts * CAP, width_model)
    picked = (
        jnp.take(flat_results, slot_index, axis=0)
        .reshape(own_tokens, TOPK, width_model)
        .astype(jnp.float32)
    )
    return jnp.sum(mixing[..., None] * picked, axis=1).astype(jnp.bfloat16)


def compose(earlier, latter):
    joined_map = jnp.einsum("hij,hjk->hik", latter[0], earlier[0], precision=precise_setting)
    joined_state = (
        jnp.einsum("hij,hjv->hiv", latter[0], earlier[1], precision=precise_setting) + latter[1]
    )
    return (joined_map, joined_state)


def shards(
    query_heads_rows,
    key_heads_rows,
    value_heads_rows,
    write_strength_logit,
    decay_preactivation,
    head_decay_logarithm,
    extra_log_decay,
    output_weight,
    second_batch_tokens,
    expert_norm_scale,
    expert_choice_index,
    group_router_weight,
    expert_logit_difference,
    expert_gate_weight,
    expert_up_weight,
    expert_down_weight,
):
    length = query_heads_rows.shape[0]
    local_heads = head_decay_logarithm.shape[0]
    strength = jax.nn.sigmoid(write_strength_logit.astype(jnp.float32))
    decay_logarithm = (
        -jnp.exp(head_decay_logarithm)[:, None]
        * jax.nn.softplus(decay_preactivation.astype(jnp.float32))
        + extra_log_decay
    )
    local_output, projection_matrix, end_memory = delta_rule(
        query_heads_rows, key_heads_rows, value_heads_rows, strength, decay_logarithm
    )
    identity_map = jnp.broadcast_to(jnp.eye(DK, dtype=jnp.float32), (local_heads, DK, DK))
    carried_end = end_memory[..., :DV]
    transfer = end_memory[..., DV:]
    _, incoming_rows = prefix(
        (transfer, carried_end), "ep", compose, (identity_map, jnp.zeros_like(carried_end))
    )
    attention_result = local_output + jnp.einsum(
        "hpg,hgd->hpd", projection_matrix, incoming_rows, precision=precise_setting
    )
    attn_rows = (
        attention_result.transpose(1, 0, 2)
        .reshape(length, local_heads * DV)
        .astype(jnp.bfloat16)
    )
    summed = lax.psum_scatter(
        jnp.dot(attn_rows, output_weight, preferred_element_type=jnp.float32).astype(jnp.bfloat16),
        "tp",
        scatter_dimension=0,
        tiled=True,
    )
    widened = second_batch_tokens.astype(jnp.float32)
    normed = (
        widened
        * lax.rsqrt(jnp.mean(widened * widened, axis=-1, keepdims=True) + norm_eps)
        * expert_norm_scale
    ).astype(jnp.bfloat16)
    leading = jax.nn.sigmoid(expert_logit_difference)
    mixing = group_router_weight[:, None] * jnp.stack([leading, 1.0 - leading], axis=-1)
    local_experts, local_units, _ = expert_gate_weight.shape
    own_tokens = second_batch_tokens.shape[0]
    ep_count, tp_count = lax.axis_size("ep"), lax.axis_size("tp")
    named_both = TOPK if local_experts % EPG == 0 else 1
    slots = min(own_tokens, local_experts * CAP // named_both)
    weights = (expert_gate_weight, expert_up_weight, expert_down_weight)
    if 2 * tp_count * ep_count * slots < 3 * local_experts * local_units * tp_count:
        expert_out = by_tokens(normed, expert_choice_index, mixing, *weights, slots)
    else:
        expert_out = by_weights(normed, expert_choice_index, mixing, *weights)
    return (summed, expert_out)


def solution(mesh):
    in_specs = (
        P("ep", "tp"),
        P("ep", "tp"),
        P("ep", "tp"),
        P("tp", "ep"),
        P("tp", "ep"),
        P("tp"),
        P("tp", "ep"),
        P("tp", None),
        P(("ep", "tp"), None),
        P(),
        P(("ep", "tp"), None),
        P(("ep", "tp")),
        P(("ep", "tp")),
        P("ep", "tp", None),
        P("ep", "tp", None),
        P("ep", "tp", None),
    )
    out_specs = (P(("ep", "tp"), None), P(("ep", "tp"), None))
    return jax.shard_map(shards, mesh=mesh, in_specs=in_specs, out_specs=out_specs, check_vma=False)
```

```python
import functools

import jax
import jax.numpy as jnp
from jax import lax
from jax.experimental import pallas as pl
from jax.experimental.pallas import tpu as pltpu
from jax.sharding import PartitionSpec as P

DK = 128
DV = 128
CAP = 32
RING = 4
MESH = pl.DeviceIdType.MESH
EPG = 4
TOPK = 2


precise_setting = lax.Precision.HIGHEST
norm_eps = 1e-06


def incoming(end_memory, axis):
    count, mine = (lax.axis_size(axis), lax.axis_index(axis))
    pieces = lax.all_gather(end_memory, axis)
    state = jnp.zeros(end_memory.shape[:-1] + (DV,), jnp.float32)
    for position in range(count - 1):
        end, transfer = pieces[position, ..., :DV], pieces[position, ..., DV:]
        longer = end + jnp.einsum("hij,hjv->hiv", transfer, state, precision=precise_setting)
        state = jnp.where(position < mine, longer, state)
    return state


def unit_rows(matrix):
    return matrix * lax.rsqrt(jnp.sum(matrix * matrix, axis=-1, keepdims=True) + norm_eps)


def mm(a, b, dims=((1,), (0,))):
    return lax.dot_general(
        a, b, (dims, ((), ())), precision=precise_setting, preferred_element_type=jnp.float32
    )


def delta_kernel(q_ref, k_ref, v_ref, strength_ref, decay_ref, local_ref, proj_ref, end_ref):
    heads = strength_ref.shape[0]
    chunk = DK
    chunks = q_ref.shape[0] // chunk
    rows = lax.broadcasted_iota(jnp.int32, (chunk, chunk), 0)
    cols = lax.broadcasted_iota(jnp.int32, (chunk, chunk), 1)
    within = rows >= cols
    eye = jnp.where(rows == cols, 1.0, 0.0)
    parts = []
    for h in range(heads):
        for c in range(chunks):
            at = pl.ds(c * chunk, chunk)
            q = q_ref[at, h * DK : (h + 1) * DK].astype(jnp.float32)
            k = k_ref[at, h * DK : (h + 1) * DK].astype(jnp.float32)
            v = v_ref[at, h * DV : (h + 1) * DV].astype(jnp.float32)
            q = unit_rows(q) * DK ** (-0.5)
            k = unit_rows(k)
            d_row = decay_ref[h : h + 1, c * chunk : (c + 1) * chunk]
            b_row = strength_ref[h : h + 1, c * chunk : (c + 1) * chunk]
            d_col = jnp.sum(jnp.where(rows == cols, d_row, 0.0), axis=1, keepdims=True)
            b_col = jnp.sum(jnp.where(rows == cols, b_row, 0.0), axis=1, keepdims=True)
            cum_col = jnp.sum(jnp.where(within, d_row, 0.0), axis=1, keepdims=True)
            cum_row = jnp.sum(jnp.where(rows <= cols, d_col, 0.0), axis=0, keepdims=True)
            last = cum_col[chunk - 1 : chunk, :]
            decayed = jnp.where(within, jnp.exp(jnp.where(within, cum_col - cum_row, 0.0)), 0.0)
            weighted = k * b_col
            lower = jnp.where(
                rows > cols, mm(weighted, k, ((1,), (1,))) * decayed, 0.0
            )
            scores = mm(q, k, ((1,), (1,))) * decayed
            grown = jnp.exp(cum_col)
            rhs = jnp.concatenate([v * b_col, weighted * grown], axis=1)
            parts.append([lower, scores, rhs, q * grown, k * jnp.exp(last - cum_col), jnp.exp(last)])
    inverses = [None] * len(parts)
    span = 1
    while span < chunk:
        mask = (
            (rows // (2 * span) == cols // (2 * span))
            & (rows // span % 2 == 1)
            & (cols // span % 2 == 0)
        )
        for i, part in enumerate(parts):
            edge = jnp.where(mask, part[0], 0.0)
            if span == 1:
                inverses[i] = eye - edge
            else:
                inverses[i] = inverses[i] - mm(mm(inverses[i], edge), inverses[i])
        span *= 2
    solved = [mm(inverse, part[2]) for inverse, part in zip(inverses, parts)]
    states = [
        jnp.concatenate([jnp.zeros((DK, DV), jnp.float32), eye], axis=1) for _ in range(heads)
    ]
    for c in range(chunks):
        for h in range(heads):
            _, scores, _, queries, keys, retention = parts[h * chunks + c]
            both = solved[h * chunks + c]
            fresh = jnp.concatenate([both[:, :DV], jnp.zeros((chunk, DK), jnp.float32)], axis=1)
            state = states[h]
            updates = fresh - mm(both[:, DV:], state)
            out = mm(queries, state) + mm(scores, updates)
            states[h] = state * retention + mm(keys, updates, ((0,), (0,)))
            at = pl.ds(c * chunk, chunk)
            local_ref[h, at, :] = out[:, :DV]
            proj_ref[h, at, :] = out[:, DV:]
    for h in range(heads):
        end_ref[h] = states[h]


def delta_rule(queries, keys, values, strength, decay_logarithm):
    heads, length = strength.shape
    vmem = pl.BlockSpec(memory_space=pltpu.VMEM)
    f32 = jnp.float32
    return pl.pallas_call(
        delta_kernel,
        out_shape=(
            jax.ShapeDtypeStruct((heads, length, DV), f32),
            jax.ShapeDtypeStruct((heads, length, DK), f32),
            jax.ShapeDtypeStruct((heads, DK, DV + DK), f32),
        ),
        in_specs=[vmem] * 5,
        out_specs=(vmem,) * 3,
        cost_estimate=pl.CostEstimate(
            flops=40 * heads * length * DK * DK * 6, bytes_accessed=4 * 2**20, transcendentals=0
        ),
        compiler_params=pltpu.CompilerParams(vmem_limit_bytes=40 * 2**20),
    )(queries, keys, values, strength, decay_logarithm)


def expert_kernel(x_ref, gate_ref, up_ref, down_ref, out_ref):
    experts, units, width = gate_ref.shape
    x = x_ref[:, :width]
    hidden = []
    for e in range(experts):
        gating = lax.dot_general(
            x, gate_ref[e], (((1,), (1,)), ((), ())), preferred_element_type=jnp.float32
        )
        upward = lax.dot_general(
            x, up_ref[e], (((1,), (1,)), ((), ())), preferred_element_type=jnp.float32
        )
        share = x_ref[:, width + e : width + e + 1].astype(jnp.float32) + x_ref[
            :, width + experts + e : width + experts + e + 1
        ].astype(jnp.float32)
        hidden.append((gating / (1.0 + jnp.exp(-gating)) * upward * share).astype(jnp.bfloat16))
    hidden = jnp.concatenate(hidden, axis=1)
    down = down_ref[...].reshape(experts * units, width)
    out_ref[...] = jnp.dot(hidden, down, preferred_element_type=jnp.float32).astype(jnp.bfloat16)


def expert_layer(rows, gate, up, down, tile):
    count, wide = rows.shape
    experts, units, width = gate.shape
    whole = pl.BlockSpec((experts, units, width), lambda i: (0, 0, 0))
    return pl.pallas_call(
        expert_kernel,
        grid=(count // tile,),
        out_shape=jax.ShapeDtypeStruct((count, width), jnp.bfloat16),
        in_specs=[pl.BlockSpec((tile, wide), lambda i: (i, 0)), whole, whole, whole],
        out_specs=pl.BlockSpec((tile, width), lambda i: (i, 0)),
        cost_estimate=pl.CostEstimate(
            flops=6 * count * experts * units * width,
            bytes_accessed=4 * count * width + 6 * experts * units * width,
            transcendentals=0,
        ),
        compiler_params=pltpu.CompilerParams(vmem_limit_bytes=48 * 2**20),
    )(rows, gate, up, down)


def exchange_kernel(
    ring, out_ref, spread_ref, gate_ref, up_ref, down_ref, result_ref,
    rows, part, theirs, pair, passed, landed, onward, total, back,
    local_sem, ep_sems, near_sems, far_sems, core_sems, pair_sems, half_sems, back_sems,
):
    e, t = lax.axis_index("ep"), lax.axis_index("tp")
    peers, slots, _ = out_ref.shape
    experts, units, width = gate_ref.shape
    half = width // 2
    core, z = lax.rem(t, 2), lax.div(t, 2)
    bf16, f32 = jnp.bfloat16, jnp.float32

    def at_chip(hop, same=True):
        return lax.rem(z + hop, ring) * 2 + (core if same else 1 - core)

    right, left, other = at_chip(1), at_chip(ring - 1), at_chip(0, False)

    def at_peer(j):
        return lax.rem(e + j, peers)

    barrier = pltpu.get_barrier_semaphore()
    greeted = [(at_peer(j), t) for j in range(1, peers)] + [(e, right), (e, left), (e, other)]
    for device in greeted:
        pl.semaphore_signal(barrier, inc=1, device_id=device, device_id_type=MESH)
    pl.semaphore_wait(barrier, len(greeted))

    started = []

    def send(src, dst, sems, index, device):
        copy = pltpu.make_async_remote_copy(
            src_ref=src,
            dst_ref=dst,
            send_sem=sems.at[(0,) + index],
            recv_sem=sems.at[(1,) + index],
            device_id=device,
            device_id_type=MESH,
        )
        copy.start()
        started.append(copy)

    def arrived(dst, sems, index):
        pltpu.make_async_remote_copy(
            src_ref=dst,
            dst_ref=dst,
            send_sem=sems.at[(0,) + index],
            recv_sem=sems.at[(1,) + index],
            device_id=(e, other),
            device_id_type=MESH,
        ).wait_recv()

    own = pltpu.make_async_copy(out_ref.at[e], rows.at[t, e], local_sem)
    own.start()
    for j in range(1, peers):
        target = at_peer(j)
        send(out_ref.at[target], rows.at[t, e], ep_sems, (j,), (target, t))
    sources = [lax.rem(e + peers - j, peers) for j in range(peers)]

    def piece(hop, j, same=True):
        return rows.at[at_chip(hop, same), sources[j]]

    def to_other(hop, j):
        send(piece(hop, j), piece(hop, j), core_sems, (hop, j), (e, other))

    def own_piece(j):
        if j == 0:
            own.wait()
        else:
            arrived(piece(0, j), ep_sems, (j,))
        send(piece(0, j), piece(0, j), near_sems, (0, j), (e, right))
        send(piece(0, j), piece(0, j), near_sems, (1, j), (e, left))
        to_other(0, j)

    def near_piece(j):
        arrived(piece(ring - 1, j), near_sems, (0, j))
        if j % 2 == 0:
            send(piece(ring - 1, j), piece(ring - 1, j), far_sems, (j,), (e, right))
        arrived(piece(1, j), near_sems, (1, j))
        if j % 2 == 1:
            send(piece(1, j), piece(1, j), far_sems, (j,), (e, left))
        to_other(ring - 1, j)
        to_other(1, j)

    def far_piece(j):
        arrived(piece(2, j), far_sems, (j,))
        to_other(2, j)

    def produce(hop):
        for j in range(peers):
            arrived(piece(hop, j, False), core_sems, (hop, j))

        def one(k, carry):
            which = lax.rem(core + 1 + k, 2)
            block = rows[lax.rem(z + hop, ring) * 2 + which].reshape(peers * slots, -1)
            x = block[:, :width]
            hidden = []
            for n in range(experts):
                gating = lax.dot_general(
                    x, gate_ref[n], (((1,), (1,)), ((), ())), preferred_element_type=f32
                )
                upward = lax.dot_general(
                    x, up_ref[n], (((1,), (1,)), ((), ())), preferred_element_type=f32
                )
                share = block[:, width + n : width + n + 1].astype(f32) + block[
                    :, width + experts + n : width + experts + n + 1
                ].astype(f32)
                hidden.append((gating / (1.0 + jnp.exp(-gating)) * upward * share).astype(bf16))
            hidden = jnp.concatenate(hidden, axis=1)
            down = down_ref[...].reshape(experts * units, width)
            for h in range(2):
                part[hop, k, h] = jnp.dot(
                    hidden, down[:, h * half : (h + 1) * half], preferred_element_type=f32
                ).astype(bf16)
            return carry

        lax.fori_loop(0, 2, one, 0)
        send(part.at[hop, 0], theirs.at[hop], pair_sems, (hop,), (e, other))

    def join(hop):
        arrived(theirs.at[hop], pair_sems, (hop,))
        for h in range(2):
            pair[hop, h] = (part[hop, 1, h].astype(f32) + theirs[hop, h].astype(f32)).astype(bf16)

    for j in range(peers):
        own_piece(j)
        if j >= 1:
            near_piece(j - 1)
        if j >= 2:
            far_piece(j - 2)
    produce(0)
    near_piece(peers - 1)
    join(0)
    far_piece(peers - 2)
    produce(1)
    produce(ring - 1)
    far_piece(peers - 1)
    join(1)
    send(pair.at[1, 1], landed.at[0, 1], half_sems, (0, 1), (e, right))
    join(ring - 1)
    send(pair.at[ring - 1, 0], landed.at[1, 0], half_sems, (1, 0), (e, left))
    produce(2)
    join(2)
    send(pair.at[2, 0], passed.at[0], half_sems, (2, 0), (e, right))
    send(pair.at[2, 1], passed.at[1], half_sems, (2, 1), (e, left))
    arrived(passed.at[0], half_sems, (2, 0))
    onward[0] = (pair[1, 0].astype(f32) + passed[0].astype(f32)).astype(bf16)
    send(onward.at[0], landed.at[0, 0], half_sems, (0, 0), (e, right))
    arrived(passed.at[1], half_sems, (2, 1))
    onward[1] = (pair[ring - 1, 1].astype(f32) + passed[1].astype(f32)).astype(bf16)
    send(onward.at[1], landed.at[1, 1], half_sems, (1, 1), (e, left))
    for h in range(2):
        arrived(landed.at[h, 1 - h], half_sems, (h, 1 - h))
    for h in range(2):
        arrived(landed.at[h, h], half_sems, (h, h))
        summed = pair[0, h].astype(f32) + landed[0, h].astype(f32) + landed[1, h].astype(f32)
        total[h] = summed.astype(bf16).reshape(peers, slots, half)
        for j in range(1, peers):
            target = at_peer(j)
            send(total.at[h, target], back.at[h, e], back_sems, (h, j), (target, t))
        back[h, e] = total[h, e]
    for h in range(2):
        for j in range(1, peers):
            arrived(back.at[h, sources[j]], back_sems, (h, j))
        result_ref[:, h * half : (h + 1) * half] = jnp.dot(
            spread_ref[...], back[h].reshape(peers * slots, half), preferred_element_type=f32
        ).astype(bf16)
    for copy in started:
        copy.wait_send()


def exchange(outgoing, spread, gate, up, down, ring):
    peers, slots, wide = outgoing.shape
    _, _, width = gate.shape
    count, half = peers * slots, width // 2
    bf16 = jnp.bfloat16
    vmem = pl.BlockSpec(memory_space=pltpu.VMEM)
    dma = pltpu.SemaphoreType.DMA
    experts, units, _ = gate.shape
    total_rows = 2 * ring * count
    return pl.pallas_call(
        functools.partial(exchange_kernel, ring),
        out_shape=jax.ShapeDtypeStruct((spread.shape[0], width), bf16),
        in_specs=[vmem] * 5,
        out_specs=vmem,
        scratch_shapes=[
            pltpu.VMEM((2 * ring, peers, slots, wide), bf16),
            pltpu.VMEM((ring, 2, 2, count, half), bf16),
            pltpu.VMEM((ring, 2, count, half), bf16),
            pltpu.VMEM((ring, 2, count, half), bf16),
            pltpu.VMEM((2, count, half), bf16),
            pltpu.VMEM((2, 2, count, half), bf16),
            pltpu.VMEM((2, count, half), bf16),
            pltpu.VMEM((2, peers, slots, half), bf16),
            pltpu.VMEM((2, peers, slots, half), bf16),
            dma,
            dma((2, peers)),
            dma((2, 2, peers)),
            dma((2, peers)),
            dma((2, ring, peers)),
            dma((2, ring)),
            dma((2, 3, 2)),
            dma((2, 2, peers)),
        ],
        cost_estimate=pl.CostEstimate(
            flops=60 * total_rows * experts * units * width,
            bytes_accessed=6 * experts * units * width,
            transcendentals=0,
        ),
        compiler_params=pltpu.CompilerParams(
            collective_id=0, has_side_effects=True, vmem_limit_bytes=60 * 2**20
        ),
    )(outgoing, spread, gate, up, down)


def by_tokens(normed, choice, mixing, gate, up, down, slots, after):
    ep_count = lax.axis_size("ep")
    local_experts = gate.shape[0]
    tokens, width = normed.shape
    bf16 = jnp.bfloat16
    f32 = jnp.float32
    named = choice[:, :, None] == jnp.arange(ep_count * local_experts, dtype=jnp.int32)
    share = jnp.sum(jnp.where(named, mixing[:, :, None], 0.0), axis=1)
    goes = jnp.any(named, axis=1).reshape(tokens, ep_count, local_experts).any(axis=-1)
    earlier = jnp.tril(jnp.ones((tokens, tokens), bf16), -1)
    rank = jnp.dot(earlier, goes.astype(bf16), preferred_element_type=f32)
    spread = goes[:, :, None] & (rank[:, :, None] == jnp.arange(slots, dtype=f32))
    spread = spread.astype(bf16)
    high = share.astype(bf16)
    low = (share - high.astype(f32)).astype(bf16)
    sent = jnp.einsum("tes,td->esd", spread, normed, preferred_element_type=f32).astype(bf16)
    extra = jnp.concatenate(
        [
            high.reshape(tokens, ep_count, local_experts),
            low.reshape(tokens, ep_count, local_experts),
        ],
        axis=-1,
    )
    extra = jnp.einsum("tes,tex->esx", spread, extra, preferred_element_type=f32).astype(bf16)
    pad = -extra.shape[-1] % 128
    extra = jnp.pad(extra, ((0, 0), (0, 0), (0, pad)))
    outgoing = jnp.concatenate([sent, extra], axis=-1)
    if lax.axis_size("tp") == 2 * RING and ep_count > 1:
        outgoing, after = lax.optimization_barrier((outgoing, after))
        flat = spread.reshape(tokens, ep_count * slots)
        return exchange(outgoing, flat, gate, up, down, RING), after
    arrived = lax.all_to_all(outgoing, "ep", split_axis=0, concat_axis=0, tiled=True)
    arrived = arrived.reshape(ep_count * slots, -1)
    everyone = lax.all_gather(arrived, "tp", axis=0, tiled=True)
    produced = expert_layer(everyone, gate, up, down, arrived.shape[0])
    summed = lax.psum_scatter(produced, "tp", scatter_dimension=0, tiled=True)
    returned = lax.all_to_all(
        summed.reshape(ep_count, slots, width), "ep", split_axis=0, concat_axis=0, tiled=True
    )
    combined = jnp.einsum("tes,esd->td", spread, returned, preferred_element_type=f32)
    return combined.astype(bf16), after


def by_weights(normed, expert_choice_index, mixing, gate, up, down):
    own_tokens, width_model = normed.shape
    ep_count = lax.axis_size("ep")
    local_experts = gate.shape[0]
    experts = local_experts * ep_count
    flat_ids = expert_choice_index.reshape(-1)
    one_hot = (flat_ids[:, None] == jnp.arange(experts, dtype=jnp.int32)[None, :]).astype(jnp.int32)
    slot_rank = jnp.sum((jnp.cumsum(one_hot, axis=0) - one_hot) * one_hot, axis=1)
    slot_index = flat_ids * CAP + slot_rank
    copy_token = jnp.arange(flat_ids.shape[0], dtype=jnp.int32) // TOPK
    slot_token = jnp.full((experts * CAP,), own_tokens, jnp.int32).at[slot_index].set(copy_token)
    outgoing = jnp.take(normed, slot_token, axis=0, mode="fill", fill_value=0).reshape(
        ep_count, local_experts, CAP, width_model
    )
    arrived = lax.all_to_all(outgoing, "ep", split_axis=0, concat_axis=0, tiled=True)
    gate_piece = lax.all_gather(gate, "tp", axis=1, tiled=True)
    up_piece = lax.all_gather(up, "tp", axis=1, tiled=True)
    down_piece = lax.all_gather(down, "tp", axis=1, tiled=True)
    gating = jnp.einsum("secd,efd->secf", arrived, gate_piece, preferred_element_type=jnp.float32)
    upward = jnp.einsum("secd,efd->secf", arrived, up_piece, preferred_element_type=jnp.float32)
    hidden = (jax.nn.silu(gating) * upward).astype(jnp.bfloat16)
    produced = jnp.einsum("secf,efd->secd", hidden, down_piece, preferred_element_type=jnp.float32)
    returned = lax.all_to_all(
        produced.astype(jnp.bfloat16), "ep", split_axis=0, concat_axis=0, tiled=True
    )
    flat_results = returned.reshape(experts * CAP, width_model)
    picked = (
        jnp.take(flat_results, slot_index, axis=0)
        .reshape(own_tokens, TOPK, width_model)
        .astype(jnp.float32)
    )
    return jnp.sum(mixing[..., None] * picked, axis=1).astype(jnp.bfloat16)


def shards(
    query_heads_rows,
    key_heads_rows,
    value_heads_rows,
    write_strength_logit,
    decay_preactivation,
    head_decay_logarithm,
    extra_log_decay,
    output_weight,
    second_batch_tokens,
    expert_norm_scale,
    expert_choice_index,
    group_router_weight,
    expert_logit_difference,
    expert_gate_weight,
    expert_up_weight,
    expert_down_weight,
):
    length = query_heads_rows.shape[0]
    local_heads = head_decay_logarithm.shape[0]
    strength = jax.nn.sigmoid(write_strength_logit.astype(jnp.float32))
    decay_logarithm = (
        -jnp.exp(head_decay_logarithm)[:, None]
        * jax.nn.softplus(decay_preactivation.astype(jnp.float32))
        + extra_log_decay
    )
    local_output, projection_matrix, end_memory = delta_rule(
        query_heads_rows, key_heads_rows, value_heads_rows, strength, decay_logarithm
    )
    incoming_rows = incoming(end_memory, "ep")
    attention_result = local_output + jnp.einsum(
        "hpg,hgd->hpd", projection_matrix, incoming_rows, precision=precise_setting
    )
    attn_rows = (
        attention_result.transpose(1, 0, 2)
        .reshape(length, local_heads * DV)
        .astype(jnp.bfloat16)
    )
    product = jnp.dot(attn_rows, output_weight, preferred_element_type=jnp.float32)
    product = product.astype(jnp.bfloat16)
    widened = second_batch_tokens.astype(jnp.float32)
    normed = (
        widened
        * lax.rsqrt(jnp.mean(widened * widened, axis=-1, keepdims=True) + norm_eps)
        * expert_norm_scale
    ).astype(jnp.bfloat16)
    leading = jax.nn.sigmoid(expert_logit_difference)
    mixing = group_router_weight[:, None] * jnp.stack([leading, 1.0 - leading], axis=-1)
    local_experts, local_units, _ = expert_gate_weight.shape
    own_tokens = second_batch_tokens.shape[0]
    ep_count, tp_count = lax.axis_size("ep"), lax.axis_size("tp")
    named_both = TOPK if local_experts % EPG == 0 else 1
    slots = min(own_tokens, local_experts * CAP // named_both)
    weights = (expert_gate_weight, expert_up_weight, expert_down_weight)
    if 2 * tp_count * ep_count * slots < 3 * local_experts * local_units * tp_count:
        expert_out, product = by_tokens(
            normed, expert_choice_index, mixing, *weights, slots, product
        )
    else:
        expert_out = by_weights(normed, expert_choice_index, mixing, *weights)
    summed = lax.psum_scatter(product, "tp", scatter_dimension=0, tiled=True)
    return (summed, expert_out)


def solution(mesh):
    in_specs = (
        P("ep", "tp"),
        P("ep", "tp"),
        P("ep", "tp"),
        P("tp", "ep"),
        P("tp", "ep"),
        P("tp"),
        P("tp", "ep"),
        P("tp", None),
        P(("ep", "tp"), None),
        P(),
        P(("ep", "tp"), None),
        P(("ep", "tp")),
        P(("ep", "tp")),
        P("ep", "tp", None),
        P("ep", "tp", None),
        P("ep", "tp", None),
    )
    out_specs = (P(("ep", "tp"), None), P(("ep", "tp"), None))
    return jax.shard_map(shards, mesh=mesh, in_specs=in_specs, out_specs=out_specs, check_vma=False)
```
